32 devices in a mesh: fs: 8 (over z, core), tp: 4 (over y, x).
Axes of the slice: x: 2, y: 2, z: 4, core: 2. Of those that a mesh axis runs over, the one named last changes fastest.
Arguments:
- saved_input: bfloat16 [6144, 2048], P('fs'), may hold values from -6 to 6
- query_cot: bfloat16 [6144, 2048], P('fs', 'tp'), may hold values from -120 to 120
- head_out: bfloat16 [6144, 2048], P('fs', 'tp'), may hold values from -120 to 120
- output_cot: bfloat16 [6144, 2048], P('fs'), may hold values from -6 to 6
- basis_q: bfloat16 [2048, 128], replicated, may hold values from -0.125 to 0.125
- basis_o: bfloat16 [2048, 128], replicated, may hold values from -0.125 to 0.125
- weight_q: float32 [2048, 2048], P('fs', 'tp'), may hold values from -0.125 to 0.125
- weight_o: float32 [2048, 2048], P('tp', 'fs'), may hold values from -0.125 to 0.125
- first_q: float32 [128, 2048], P(None, 'tp'), may hold values from -2 to 2
- second_q: float32 [128, 2048], P(None, 'tp'), may hold values from 0.01 to 1
- first_o: float32 [2048, 128], P('tp'), may hold values from -2 to 2
- second_o: float32 [2048, 128], P('tp'), may hold values from 0.01 to 1
Outputs:
- step_q: float32 [2048, 2048], P('fs', 'tp')
- step_o: float32 [2048, 2048], P('tp', 'fs')
- new_weight_q: float32 [2048, 2048], P('fs', 'tp')
- new_weight_o: float32 [2048, 2048], P('tp', 'fs')
- copy_q: bfloat16 [2048, 2048], P(None, 'tp')
- copy_o: bfloat16 [2048, 2048], P('tp')
- moment_q: float32 [128, 2048], P(None, 'tp')
- square_q: float32 [128, 2048], P(None, 'tp')
- moment_o: float32 [2048, 128], P('tp')
- square_o: float32 [2048, 128], P('tp')
The draws below stay inside these ranges and needn't reach their ends.
All inputs are finite; a program needn't handle non-finite values.
Results may differ from the reference program's by a relative error of at most 0.0035.
Values may be sent and summed in bfloat16 or wider, within the bound.
No kernel may reach another device: no remote copies, remote signals or barrier semaphores. Data moves between devices by JAX's collectives and lax.ppermute only.
A program may use at most 64 MiB of HBM per device.

```python
import math
import jax
import jax.numpy as jnp
from jax import lax

D = 2048
HEADS = 16
HEAD = 128
RANK = 128
TOKENS = 6144
QDIM = 2048


def scaled_columns(key, salt):
    key = jax.random.fold_in(key, salt)
    drawn_key, column_key = jax.random.split(key, 2)
    full_width = HEADS * HEAD
    head_number = (jnp.arange(full_width) // HEAD).astype(jnp.float32)
    head_rise = 3.0 ** (head_number / max(HEADS - 1, 1))
    column_spread = 10.0 ** jax.random.uniform(column_key, (full_width,), jnp.float32)
    drawn_draw = jnp.clip(jax.random.normal(drawn_key, (TOKENS, full_width), jnp.float32), -4.0, 4.0)
    return (drawn_draw * head_rise * column_spread).astype(jnp.bfloat16)


def draw_query_cot(key, part):
    return scaled_columns(key, 11)


def draw_head_out(key, part):
    return scaled_columns(key, 23)


def strengthened(values, rng, source, target, shards_of, factor):
    def block_of(position):
        return (jnp.arange(values.shape[position]) // (values.shape[position] // shards_of)).reshape((-1,) + (1,) * (values.ndim - 1 - position))

    near = jax.random.permutation(rng, shards_of)[block_of(target)]
    other_side = (block_of(target) + shards_of // 2) % shards_of
    return jnp.where((block_of(source) == near) | (block_of(source) == other_side), factor * values, values)


def level_of(rng, shape, shards, least, top_value):
    def one(dim, parts):
        draws = jax.random.uniform(jax.random.fold_in(jax.random.fold_in(rng, 6), dim), (parts,), jnp.float32, least / len(shards), top_value / len(shards))
        return jnp.repeat(jnp.exp(draws), shape[dim] // parts).reshape((-1,) + (1,) * (len(shape) - dim - 1))

    level = one(*shards[0])
    for cut in shards[1:]:
        level = level * one(*cut)
    return level


def centred(stream_key, extent, width, most, cuts=(), held_as=jnp.bfloat16):
    drawn = width * jax.random.normal(stream_key, extent, jnp.float32)
    if cuts:
        drawn = drawn * level_of(stream_key, extent, cuts, -0.22, 0.18)
    return jnp.clip(drawn, -most, most).astype(held_as)


def noise_with(key, extent, scale, bound, cuts, heavy, kind=jnp.bfloat16):
    entries = scale * jax.random.normal(key, extent, jnp.float32)
    if cuts:
        entries = entries * level_of(key, extent, cuts, -0.22, 0.18)
    return jnp.clip(strengthened(entries, jax.random.fold_in(key, 3), *heavy), -bound, bound).astype(kind)


def setup_inputs(seed: int = 0) -> dict:
    arg_keys = jax.random.split(jax.random.key(seed), 13)
    return {
        "saved_input": noise_with(arg_keys[0], (TOKENS, D), 1.0, 6.0, ((0, 8),), (0, 1, 8, 2.0)),
        "query_cot": draw_query_cot(jax.random.fold_in(arg_keys[12], 71), 0),
        "head_out": draw_head_out(jax.random.fold_in(arg_keys[12], 71), 0),
        "output_cot": noise_with(arg_keys[3], (TOKENS, D), 1.0, 6.0, ((0, 8),), (0, 1, 8, 2.0)),
        "basis_q": centred(arg_keys[4], (D, RANK), D ** -0.5, 0.125),
        "basis_o": centred(arg_keys[5], (D, RANK), D ** -0.5, 0.125),
        "weight_q": centred(arg_keys[6], (D, QDIM), D ** -0.5, 0.125, ((0, 8), (1, 4)), jnp.float32),
        "weight_o": centred(arg_keys[7], (QDIM, D), QDIM ** -0.5, 0.125, ((0, 4), (1, 8)), jnp.float32),
        "first_q": centred(arg_keys[8], (RANK, QDIM), 0.3, 2.0, ((1, 4),), jnp.float32),
        "second_q": jnp.clip(jnp.exp(math.log(1.0) - 4.6051702 * jax.random.uniform(arg_keys[9], (RANK, QDIM), jnp.float32) ** level_of(arg_keys[9], (RANK, QDIM), ((1, 4),), -0.2, 0.2)), 0.01, 1.0),
        "first_o": centred(arg_keys[10], (QDIM, RANK), 0.3, 2.0, ((0, 4),), jnp.float32),
        "second_o": jnp.clip(jnp.exp(math.log(1.0) - 4.6051702 * jax.random.uniform(arg_keys[11], (QDIM, RANK), jnp.float32) ** level_of(arg_keys[11], (QDIM, RANK), ((0, 4),), -0.2, 0.2)), 0.01, 1.0),
    }


BETA_FIRST = 0.9
BETA_SECOND = 0.95
ADAM_EPS = 1e-08
NORM_EPS = 1e-06
CLIP_RMS = 1.0
LEARN_RATE = 0.01

def reference(saved_input, query_cot, head_out, output_cot, basis_q, basis_o, weight_q, weight_o, first_q, second_q, first_o, second_o):
    highest = lax.Precision.HIGHEST
    grad_q = jnp.dot(saved_input.T, query_cot, preferred_element_type=jnp.float32)
    grad_o = jnp.dot(head_out.T, output_cot, preferred_element_type=jnp.float32)
    low_q = jnp.dot(basis_q.astype(jnp.float32).T, grad_q, precision=highest)
    low_o = jnp.dot(grad_o, basis_o.astype(jnp.float32), precision=highest)
    square_total = jnp.sum(low_q * low_q) + jnp.sum(low_o * low_o)
    rms_value = jnp.sqrt(square_total / (2 * RANK * HEADS * HEAD) + NORM_EPS)
    factor = jnp.minimum(1.0, CLIP_RMS / rms_value)
    moment_q = BETA_FIRST * first_q + (1.0 - BETA_FIRST) * factor * low_q
    square_q = BETA_SECOND * second_q + (1.0 - BETA_SECOND) * (factor * low_q) ** 2
    moment_o = BETA_FIRST * first_o + (1.0 - BETA_FIRST) * factor * low_o
    square_o = BETA_SECOND * second_o + (1.0 - BETA_SECOND) * (factor * low_o) ** 2
    dir_q = moment_q / (jnp.sqrt(square_q) + ADAM_EPS)
    dir_o = moment_o / (jnp.sqrt(square_o) + ADAM_EPS)
    step_q = jnp.dot(basis_q.astype(jnp.float32), dir_q, precision=highest)
    step_o = jnp.dot(dir_o, basis_o.astype(jnp.float32).T, precision=highest)
    new_weight_q = weight_q - LEARN_RATE * step_q
    new_weight_o = weight_o - LEARN_RATE * step_o
    return (step_q, step_o, new_weight_q, new_weight_o, new_weight_q.astype(jnp.bfloat16), new_weight_o.astype(jnp.bfloat16), moment_q, square_q, moment_o, square_o)
```

```python
import jax
import jax.numpy as jnp
from jax import lax
from jax.sharding import PartitionSpec as P

HEADS = 16
HEAD = 128
RANK = 128


BETA_FIRST = 0.9
BETA_SECOND = 0.95
ADAM_EPS = 1e-08
NORM_EPS = 1e-06
CLIP_RMS = 1.0
LEARN_RATE = 0.01
WIRE_SCALE = 65536.0


def split_product(factor_part, data_part):
    upper = factor_part.astype(jnp.bfloat16)
    lower = (factor_part - upper.astype(jnp.float32)).astype(jnp.bfloat16)
    first = jnp.dot(upper, data_part, preferred_element_type=jnp.float32)
    return first + jnp.dot(lower, data_part, preferred_element_type=jnp.float32)


def basis_product(basis, direction):
    upper = direction.astype(jnp.bfloat16)
    lower = (direction - upper.astype(jnp.float32)).astype(jnp.bfloat16)
    first = jnp.dot(basis, upper, preferred_element_type=jnp.float32)
    return first + jnp.dot(basis, lower, preferred_element_type=jnp.float32)


def to_wire(weight):
    return (weight * WIRE_SCALE).astype(jnp.float16)


def from_wire(block):
    return block.astype(jnp.float32) * (1.0 / WIRE_SCALE)


def adam(first, second, low, factor):
    moment = BETA_FIRST * first + (1.0 - BETA_FIRST) * factor * low
    square = BETA_SECOND * second + (1.0 - BETA_SECOND) * (factor * low) ** 2
    return moment, square, moment / (jnp.sqrt(square) + ADAM_EPS)


def make_shards(n_fs, n_tp):
    n_z = n_fs // 2
    swap = [(2 * z + c, 2 * z + 1 - c) for z in range(n_z) for c in range(2)]

    def line(step, first, last):
        return [(2 * z + c, 2 * (z + step) + c) for z in range(first, last) for c in range(2)]

    def turn(k):
        return [(2 * z + c, 2 * ((z + k) % n_z) + c) for z in range(n_z) for c in range(2)]

    def send(value, pairs, axis="fs"):
        return lax.ppermute(value, axis, pairs)

    def gather_low(partial, z, c):
        half = partial.shape[0] // 2
        mine = lax.dynamic_slice_in_dim(partial, c * half, half, 0)
        other = lax.dynamic_slice_in_dim(partial, (1 - c) * half, half, 0)
        mine = mine + send(other, swap)
        rows = half // n_z
        chunk = lax.dynamic_slice_in_dim(mine, z * rows, rows, 0)
        for k in range(1, n_z):
            out = lax.dynamic_slice_in_dim(mine, ((z + k) % n_z) * rows, rows, 0)
            chunk = chunk + send(out, turn(k))
        whole = jnp.zeros_like(mine)
        whole = lax.dynamic_update_slice_in_dim(whole, chunk, z * rows, 0)
        for k in range(1, n_z):
            whole = lax.dynamic_update_slice_in_dim(whole, send(chunk, turn(k)), ((z - k) % n_z) * rows, 0)
        twin = send(whole, swap)
        return jnp.where(c == 0, whole, twin), jnp.where(c == 0, twin, whole)

    def tp_sum(value):
        value = jnp.full((8, 128), value)
        total = value
        for k in range(1, n_tp):
            total = total + send(value, [(i, (i + k) % n_tp) for i in range(n_tp)], "tp")
        return total[0, 0]

    def spread(own, z, dim):
        size = own.shape[dim]
        right1 = send(own, line(1, 0, 3))
        left1 = send(own, line(-1, 1, 4))
        right2 = send(right1, line(1, 1, 3))
        left2 = send(left1, line(-1, 1, 3))
        third = send(jnp.where(z == 2, right2, left2), line(1, 2, 3) + line(-1, 1, 2))
        near = jnp.where(z == 0, left1, right1)
        middle = jnp.where(z == 0, left2, jnp.where(z == 3, right2, left1))
        far = jnp.where(z == 1, left2, jnp.where(z == 2, right2, third))
        place = [
            z,
            jnp.where(z == 0, 1, z - 1),
            jnp.where(z == 0, 2, jnp.where(z == 3, 1, z + 1)),
            jnp.where(z <= 1, 3, 0),
        ]
        return [(p, b, send(b, swap)) for p, b in zip(place, (own, near, middle, far))]

    def shards(
        saved_input,
        query_cot,
        head_out,
        output_cot,
        basis_q,
        basis_o,
        weight_q,
        weight_o,
        first_q,
        second_q,
        first_o,
        second_o,
    ):
        row_count = weight_q.shape[0]
        position = lax.axis_index("fs")
        offset = position * row_count
        wire_q = to_wire(weight_q)
        wire_o = to_wire(weight_o)
        input_low = jnp.dot(saved_input, basis_q, preferred_element_type=jnp.float32)
        partial_q = split_product(input_low.T, query_cot)
        cot_low = jnp.dot(output_cot, basis_o, preferred_element_type=jnp.float32)
        partial_o = split_product(cot_low.T, head_out)
        partial = jnp.concatenate((partial_q, partial_o), 0)
        if n_z == 4:
            z, c = position // 2, position % 2
            blocks_q = spread(wire_q, z, 0)
            blocks_o = spread(wire_o, z, 1)
            low_q, low_o = gather_low(partial, z, c)
            norm = tp_sum(jnp.sum(low_q * low_q) + jnp.sum(low_o * low_o))
        else:
            summed = lax.psum_scatter(partial, "fs", scatter_dimension=0, tiled=True)
            low_q, low_o = jnp.split(lax.all_gather(summed, "fs", axis=0, tiled=True), 2, 0)
            norm = lax.psum(jnp.sum(low_q * low_q) + jnp.sum(low_o * low_o), "tp")
        low_o = low_o.T
        rms_value = jnp.sqrt(norm / (2 * RANK * HEADS * HEAD) + NORM_EPS)
        factor = jnp.minimum(1.0, CLIP_RMS / rms_value)
        moment_q, square_q, dir_q = adam(first_q, second_q, low_q, factor)
        moment_o, square_o, dir_o = adam(first_o, second_o, low_o, factor)
        full_q = basis_product(basis_q, dir_q)
        full_o = basis_product(basis_o, dir_o.T).T
        step_q = lax.dynamic_slice_in_dim(full_q, offset, row_count, 0)
        step_o = lax.dynamic_slice_in_dim(full_o, offset, row_count, 1)
        new_weight_q = weight_q - LEARN_RATE * step_q
        new_weight_o = weight_o - LEARN_RATE * step_o
        if n_z == 4:
            old_q = jnp.zeros(full_q.shape, jnp.float32)
            old_o = jnp.zeros(full_o.shape, jnp.float32)
            for place, mine, twin in blocks_q:
                start = place * 2 * row_count
                old_q = lax.dynamic_update_slice_in_dim(old_q, from_wire(mine), start + c * row_count, 0)
                old_q = lax.dynamic_update_slice_in_dim(old_q, from_wire(twin), start + (1 - c) * row_count, 0)
            for place, mine, twin in blocks_o:
                start = place * 2 * row_count
                old_o = lax.dynamic_update_slice_in_dim(old_o, from_wire(mine), start + c * row_count, 1)
                old_o = lax.dynamic_update_slice_in_dim(old_o, from_wire(twin), start + (1 - c) * row_count, 1)
        else:
            old_q = from_wire(lax.all_gather(wire_q, "fs", axis=0, tiled=True))
            old_o = from_wire(lax.all_gather(wire_o, "fs", axis=1, tiled=True))
        copy_q = (old_q - LEARN_RATE * full_q).astype(jnp.bfloat16)
        copy_o = (old_o - LEARN_RATE * full_o).astype(jnp.bfloat16)
        return (
            step_q,
            step_o,
            new_weight_q,
            new_weight_o,
            copy_q,
            copy_o,
            moment_q,
            square_q,
            moment_o,
            square_o,
        )

    return shards


def solution(mesh):
    return jax.shard_map(
        make_shards(mesh.shape["fs"], mesh.shape["tp"]),
        mesh=mesh,
        in_specs=(
            P("fs", None),
            P("fs", "tp"),
            P("fs", "tp"),
            P("fs", None),
            P(),
            P(),
            P("fs", "tp"),
            P("tp", "fs"),
            P(None, "tp"),
            P(None, "tp"),
            P("tp", None),
            P("tp", None),
        ),
        out_specs=(
            P("fs", "tp"),
            P("tp", "fs"),
            P("fs", "tp"),
            P("tp", "fs"),
            P(None, "tp"),
            P("tp", None),
            P(None, "tp"),
            P(None, "tp"),
            P("tp", None),
            P("tp", None),
        ),
        check_vma=False,
    )
```
